32 devices in a mesh: grp: 2 (over y), fs: 4 (over z), tp: 4 (over x, core).
Axes of the slice: x: 2, y: 2, z: 4, core: 2. Of those that a mesh axis runs over, the one named last changes fastest.
Arguments:
- tokens: bfloat16 [4096, 2048], P(('grp', 'fs'), 'tp'), parts along dimension 0, may hold values from -36 to 36
- query_matrix: bfloat16 [2048, 1024], P('fs', 'tp'), may hold values from -0.125 to 0.125
- key_weight: bfloat16 [2048, 1024], P('fs', 'tp'), may hold values from -0.125 to 0.125
- value_weight: bfloat16 [2048, 2048], P('fs', 'tp'), may hold values from -0.125 to 0.125
- forget_lower_factor: bfloat16 [2048, 32], replicated, may hold values from -0.125 to 0.125
- decay_up: bfloat16 [32, 1024], replicated, may hold values from -1 to 1
- decay_bias: float32 [1024], replicated, may hold values from -1 to 8
- log_extra: float32 [4096, 1024], P(('grp', 'fs'), 'tp'), parts along dimension 0, may hold values from -0.7 to 0
- head_gain: float32 [256], replicated, may hold values from 0.1 to 1.9
- out_weight: bfloat16 [2048, 2048], P('tp', 'fs'), may hold values from -0.125 to 0.125
- mix_gain: float32 [2048], P('tp'), may hold values from 0.1 to 1.9
- up_weight: bfloat16 [2048, 8192], P('fs', 'tp'), may hold values from -0.125 to 0.125
- down_weight: bfloat16 [8192, 2048], P('tp', 'fs'), may hold values from -0.0625 to 0.0625
- out_gain: float32 [2048], P('tp'), may hold values from 0.1 to 1.9
Outputs:
- layer_out: bfloat16 [4096, 2048], P(('grp', 'fs'), 'tp'), parts along dimension 0
The draws below stay inside these ranges and needn't reach their ends.
There are 2 independent parts, one for each index of `grp`. The reference program is written for one: setup_inputs(seed, part) draws one part's arguments, and reference() takes and returns one part's arrays. A program takes and returns all parts, laid end to end along the dimension named above; an argument that names none is the same for every part. Nothing has to cross between parts.
All inputs are finite; a program needn't handle non-finite values.
Results may differ from the reference program's by a relative error of at most 0.015.
Values may be sent and summed in bfloat16 or wider, within the bound.
No kernel may reach another device: no remote copies, remote signals or barrier semaphores. Data moves between devices by JAX's collectives and lax.ppermute only.
A program may use at most 64 MiB of HBM per device.

```python
import math
import jax
import jax.numpy as jnp
from jax import lax

D = 2048
HEADS = 8
DK = 128
DV = 256
FF = 8192
RANK = 32
SEGMENT_LENGTH = 64
SEQ = 512
OVERALL_WORDS = 2048
N_TP = 4


def draw_tokens(key, part):
    address_embeddings = jax.random.split(key, 3)
    column_index = jnp.arange(D).astype(jnp.float32)
    col_scale = 3.0 ** (column_index / (D - 1)) * jnp.exp(jax.random.uniform(address_embeddings[1], (D,), jnp.float32, 0.0, math.log(1.5))) / 1.5
    row_scale = jnp.exp(jax.random.uniform(address_embeddings[2], (OVERALL_WORDS, 1), jnp.float32, 0.0, math.log(2.0)))
    base = jnp.clip(jax.random.normal(address_embeddings[0], (OVERALL_WORDS, D), jnp.float32), -6.0, 6.0)
    return (base * col_scale * row_scale).astype(jnp.bfloat16)


def draw_decay_bias(key, part):
    address_embeddings = jax.random.split(key, 3)
    width = HEADS * DK
    picked = jax.random.randint(address_embeddings[0], (width,), 0, 2)
    fast = jax.random.uniform(address_embeddings[1], (width,), jnp.float32, -1.0, 1.5)
    slow = jax.random.uniform(address_embeddings[2], (width,), jnp.float32, 4.0, 7.0)
    return jnp.where(picked == 1, fast, slow)


def draw_log_extra(key, part):
    address_embeddings = jax.random.split(key, 3)
    width = HEADS * DK
    forget_speeds = jnp.exp(jax.random.uniform(address_embeddings[0], (OVERALL_WORDS // SEGMENT_LENGTH, width), jnp.float32, math.log(0.0005), math.log(0.004)))
    word_segments = jax.random.randint(address_embeddings[1], (OVERALL_WORDS, 1), 0, 128) == 0
    forget_intensity = jax.random.uniform(address_embeddings[2], (OVERALL_WORDS, width), jnp.float32, math.log(0.5), math.log(0.8))
    return -jnp.repeat(forget_speeds, SEGMENT_LENGTH, axis=0) + jnp.where(word_segments, forget_intensity, 0.0)


def block_levels(stream_key, dims, cuts, low, high):
    level, own = 1.0, jax.random.fold_in(stream_key, 6)
    for axis_at, shards_of in cuts:
        heights = jnp.exp(jax.random.uniform(jax.random.fold_in(own, axis_at), (shards_of,), jnp.float32, low / len(cuts), high / len(cuts)))
        level = level * jnp.repeat(heights, dims[axis_at] // shards_of).reshape([-1 if axis == axis_at else 1 for axis in range(len(dims))])
    return level


def noise(stream_key, shape, scale, bound, cuts=(), dtype=jnp.bfloat16):
    values = scale * jax.random.normal(stream_key, shape, jnp.float32)
    if cuts:
        values = values * block_levels(stream_key, shape, cuts, -0.22, 0.18)
    return jnp.clip(values, -bound, bound).astype(dtype)


def setup_inputs(seed: int = 0, part: int = 0) -> dict:
    keys = jax.random.split(jax.random.key(seed), 15)
    part_keys = jax.random.split(jax.random.fold_in(keys[14], part), 15)
    tokens = draw_tokens(jax.random.fold_in(jax.random.fold_in(keys[14], part), 71), part)
    query_matrix = noise(keys[1], (D, HEADS * DK), D ** -0.5, 0.125, ((0, 4), (1, 4)))
    key_weight = noise(keys[2], (D, HEADS * DK), D ** -0.5, 0.125, ((0, 4), (1, 4)))
    value_weight = noise(keys[3], (D, HEADS * DV), D ** -0.5, 0.125, ((0, 4), (1, 4)))
    forget_lower_factor = noise(keys[4], (D, RANK), D ** -0.5, 0.125)
    decay_up = noise(keys[5], (RANK, HEADS * DK), RANK ** -0.5, 1.0)
    decay_bias = draw_decay_bias(jax.random.fold_in(keys[14], 71), part)
    log_extra = draw_log_extra(jax.random.fold_in(jax.random.fold_in(keys[14], part), 71), part)
    head_gain = jnp.clip(1.0 + 0.18 * jax.random.normal(keys[8], (DV,), jnp.float32), 0.1, 1.9)
    out_weight = noise(keys[9], (HEADS * DV, D), (HEADS * DV) ** -0.5, 0.125, ((0, 4), (1, 4)))
    mix_gain = jnp.clip(1.0 + 0.18 * jax.random.normal(keys[10], (D,), jnp.float32), 0.1, 1.9)
    up_weight = noise(keys[11], (D, FF), D ** -0.5, 0.125, ((0, 4), (1, 4)))
    down_weight = noise(keys[12], (FF, D), FF ** -0.5, 0.0625, ((0, 4), (1, 4)))
    out_gain = jnp.clip(1.0 + 0.18 * jax.random.normal(keys[13], (D,), jnp.float32), 0.1, 1.9)
    return {"tokens": tokens, "query_matrix": query_matrix, "key_weight": key_weight, "value_weight": value_weight, "forget_lower_factor": forget_lower_factor, "decay_up": decay_up, "decay_bias": decay_bias, "log_extra": log_extra, "head_gain": head_gain, "out_weight": out_weight, "mix_gain": mix_gain, "up_weight": up_weight, "down_weight": down_weight, "out_gain": out_gain}


ALPHA = 2.0 ** 0.5
TAU = 16.0
EPS = 1e-05
HIGH = lax.Precision.HIGHEST

def block_scan(queries, key_rows, value_rows, log_decay):
    span = queries.shape[2]
    causal = (jnp.arange(span)[:, None] >= jnp.arange(span)[None, :])[:, :, None]

    def step(state, inputs):
        query_block, key_block, value_block, decay_block = inputs
        cumul = jnp.cumsum(decay_block, axis=1)
        last_cum = cumul[:, -1:, :]
        carried = jnp.einsum('hcd,hde->hce', query_block * jnp.exp(cumul), state, precision=HIGH)
        differ = cumul[:, :, None, :] - cumul[:, None, :, :]
        weights = jnp.exp(jnp.where(causal, differ, -jnp.inf))
        scores = lax.optimization_barrier(jnp.sum(query_block[:, :, None, :] * key_block[:, None, :, :] * weights, axis=-1))
        within = jnp.einsum('hij,hje->hie', scores, value_block, precision=HIGH)
        fresh = jnp.einsum('hcd,hce->hde', key_block * jnp.exp(last_cum - cumul), value_block, precision=HIGH)
        new_state = jnp.exp(last_cum[:, 0, :])[:, :, None] * state + fresh
        return (new_state, carried + within)
    start = jnp.zeros((queries.shape[1], queries.shape[3], value_rows.shape[3]), jnp.float32)
    _, outputs = lax.scan(step, start, (queries, key_rows, value_rows, log_decay))
    return outputs

def mixer_sequence(inputs):
    queries, key_rows, value_rows, log_decay = inputs
    count = queries.shape[0] // SEGMENT_LENGTH

    def blocks(array, depth):
        return array.astype(jnp.float32).reshape(count, SEGMENT_LENGTH, HEADS, depth).transpose(0, 2, 1, 3)
    outputs = block_scan(blocks(queries, DK) * DK ** (-0.5), blocks(key_rows, DK), blocks(value_rows, DV), blocks(log_decay, DK))
    return outputs.transpose(0, 2, 1, 3).reshape(queries.shape[0], HEADS, DV)

def group_sum(left, right, width):
    running = jnp.zeros((left.shape[0], right.shape[1]), jnp.float32)
    for index in range(N_TP):
        partial_sum = jnp.dot(left[:, index * width:(index + 1) * width], right[index * width:(index + 1) * width], preferred_element_type=jnp.float32).astype(jnp.bfloat16)
        partial_sum = lax.optimization_barrier(partial_sum)
        running = running + partial_sum.astype(jnp.float32)
    return running

def layer_norm(summed, gain_cols):
    row_mean = lax.optimization_barrier(jnp.mean(summed, axis=1, keepdims=True))
    centered = summed - row_mean
    row_var = lax.optimization_barrier(jnp.mean(centered * centered, axis=1, keepdims=True))
    return (centered * lax.rsqrt(row_var + EPS) * gain_cols).astype(jnp.bfloat16)

def reference(tokens, query_matrix, key_weight, value_weight, forget_lower_factor, decay_up, decay_bias, log_extra, head_gain, out_weight, mix_gain, up_weight, down_weight, out_gain):
    queries = jnp.dot(tokens, query_matrix, preferred_element_type=jnp.float32).astype(jnp.bfloat16)
    key_rows = jnp.dot(tokens, key_weight, preferred_element_type=jnp.float32).astype(jnp.bfloat16)
    value_rows = jnp.dot(tokens, value_weight, preferred_element_type=jnp.float32).astype(jnp.bfloat16)
    low = jnp.dot(tokens, forget_lower_factor, preferred_element_type=jnp.float32).astype(jnp.bfloat16)
    gate_pre = jnp.dot(low, decay_up, preferred_element_type=jnp.float32) + decay_bias
    log_decay = jax.nn.log_sigmoid(gate_pre) / TAU + log_extra
    count = tokens.shape[0] // SEQ
    attended = lax.map(mixer_sequence, (queries.reshape(count, SEQ, HEADS * DK), key_rows.reshape(count, SEQ, HEADS * DK), value_rows.reshape(count, SEQ, HEADS * DV), log_decay.reshape(count, SEQ, HEADS * DK)))
    attended = attended.reshape(tokens.shape[0], HEADS, DV)
    scaled = attended * lax.rsqrt(lax.optimization_barrier(jnp.mean(attended * attended, axis=-1, keepdims=True)) + EPS) * head_gain
    mixed_heads = scaled.reshape(tokens.shape[0], HEADS * DV).astype(jnp.bfloat16)
    mix = group_sum(mixed_heads, out_weight, HEADS * DV // N_TP)
    normed = layer_norm(ALPHA * tokens.astype(jnp.float32) + mix, mix_gain)
    hidden = jnp.dot(normed, up_weight, preferred_element_type=jnp.float32)
    activation = jnp.square(jax.nn.relu(hidden)).astype(jnp.bfloat16)
    down = group_sum(activation, down_weight, FF // N_TP)
    return layer_norm(ALPHA * normed.astype(jnp.float32) + down, out_gain)
```

```python
import jax
import jax.numpy as jnp
from jax import lax
from jax.experimental import pallas as pl
from jax.experimental.pallas import tpu as pltpu
from jax.sharding import PartitionSpec as P

DK = 128
DV = 256
CHUNK = 128
LEVELS = (64, 32, 16, 8)

ALPHA = 2.0**0.5
TAU = 16.0
EPS = 1e-05
CORES = 2
PAIR = 2
TILE = 256
MIB = 2**20


ANY = pl.BlockSpec(memory_space=pl.ANY)
SMEM = pl.BlockSpec(memory_space=pltpu.SMEM)
VMEM = pl.BlockSpec(memory_space=pltpu.VMEM)
NT = (((1,), (1,)), ((), ()))
TN = (((0,), (0,)), ((), ()))


def shift(array, axis, size, step):
    return lax.ppermute(array, axis, [(i, (i + step) % size) for i in range(size)])


def swap(array, axis, size):
    return lax.ppermute(array, axis, [(i, i ^ 1) for i in range(size)])


def after(array, *others):
    return lax.optimization_barrier((array, *others))[0]


def dot(left, right):
    return jnp.dot(left, right, preferred_element_type=jnp.float32)


def fetch(copies, sems):
    started = [pltpu.make_async_copy(s, d, sems.at[i]) for i, (s, d) in enumerate(copies)]
    for copy in started:
        copy.start()
    for copy in started:
        copy.wait()


def log_sigmoid(value):
    return jnp.minimum(value, 0.0) - jnp.log1p(jnp.exp(-jnp.abs(value)))


def scan_block(heads, c, states, qkv, low_ref, up_ref, bias_ref, extra_ref, gain_ref, out_ref):
    row = lax.broadcasted_iota(jnp.int32, (CHUNK, CHUNK), 0)
    col = lax.broadcasted_iota(jnp.int32, (CHUNK, CHUNK), 1)
    tri = (row >= col).astype(jnp.float32)
    row_id = lax.broadcasted_iota(jnp.int32, (CHUNK, DK), 0)
    diag_mask = (row // 8 == col // 8) & (col <= row)
    rows = pl.ds(pl.multiple_of(c * CHUNK, CHUNK), CHUNK)
    gate = dot(low_ref[rows, :], up_ref[...]) + bias_ref[...]
    decay = log_sigmoid(gate) / TAU + extra_ref[rows, :]
    cumul_all = jnp.dot(
        tri, decay, precision=lax.Precision.HIGHEST, preferred_element_type=jnp.float32
    )
    new_states = []
    for h in range(heads):
        ks = slice(h * DK, (h + 1) * DK)
        k_at = (heads + h) * DK
        v_at = 2 * heads * DK + h * DV
        cumul = cumul_all[:, ks]
        last = cumul[CHUNK - 1 : CHUNK, :]
        q = qkv[rows, ks].astype(jnp.float32) * DK ** (-0.5)
        k = qkv[rows, k_at : k_at + DK].astype(jnp.float32)
        v = qkv[rows, v_at : v_at + DV]
        state = states[h]
        scores = jnp.zeros((CHUNK, CHUNK), jnp.float32)
        for half in LEVELS:
            groups = CHUNK // (2 * half)
            mids = cumul.reshape(groups, 2 * half, DK)[:, half - 1 : half, :]
            mid = jnp.broadcast_to(mids, (groups, 2 * half, DK)).reshape(CHUNK, DK)
            upper = row_id % (2 * half) >= half
            gap = cumul - mid
            exponent = jnp.where(upper, gap, -gap)
            mixed = (jnp.where(upper, q, k) * jnp.exp(exponent)).astype(jnp.bfloat16)
            part = lax.dot_general(mixed, mixed, NT, preferred_element_type=jnp.float32)
            mask = (
                (row // (2 * half) == col // (2 * half))
                & (row % (2 * half) >= half)
                & (col % (2 * half) < half)
            )
            scores = scores + jnp.where(mask, part, 0.0)
        diag = jnp.zeros((CHUNK, CHUNK), jnp.float32)
        cumul_3d = cumul.reshape(CHUNK // 8, 8, DK)
        k_3d = k.reshape(CHUNK // 8, 8, DK)
        for j in range(8):
            base = jnp.broadcast_to(cumul_3d[:, j : j + 1, :], cumul_3d.shape).reshape(CHUNK, DK)
            key = jnp.broadcast_to(k_3d[:, j : j + 1, :], k_3d.shape).reshape(CHUNK, DK)
            term = q * key * jnp.exp(jnp.minimum(cumul - base, 0.0))
            pick = (col % 8 == j).astype(jnp.bfloat16)
            diag = diag + dot(term.astype(jnp.bfloat16), pick)
        scores = scores + jnp.where(diag_mask, diag, 0.0)
        carried = lax.dot_general(
            (q * jnp.exp(cumul)).astype(jnp.bfloat16),
            state.astype(jnp.bfloat16),
            NT,
            preferred_element_type=jnp.float32,
        )
        attended = carried + dot(scores.astype(jnp.bfloat16), v)
        fresh = lax.dot_general(
            v,
            (k * jnp.exp(last - cumul)).astype(jnp.bfloat16),
            TN,
            preferred_element_type=jnp.float32,
        )
        new_states.append(jnp.exp(last) * state + fresh)
        power = jnp.mean(attended * attended, axis=-1, keepdims=True)
        scaled = attended * lax.rsqrt(power + EPS) * gain_ref[...]
        out_ref[rows, h * DV : (h + 1) * DV] = scaled.astype(jnp.bfloat16)
    return tuple(new_states)


def pieces_of(count, n_y):
    return [(s, j) for s in range(1, count) for j in range(n_y)]


def mixer_call(place, n_y, n_z, tokens, weights, pieces, lower, up, bias, extra, gain):
    n_t = len(tokens)
    rows, width = tokens[0].shape
    heads = up.shape[1] // DK
    kb = weights[0].shape[0]
    part = kb // n_y
    cols = [w.shape[1] for w in weights]
    total = sum(cols)
    order = pieces_of(n_z, n_y)
    n_copies = n_t + len(weights) + len(order)

    def body(place_ref, *refs):
        token_refs = refs[:n_t]
        weight_refs = refs[n_t : n_t + len(cols)]
        piece_refs = refs[n_t + len(cols) : n_copies]
        lower_ref, up_ref, bias_ref, extra_ref, gain_ref, out_ref = refs[n_copies : n_copies + 6]
        x_ref, w_ref, qkv_ref, low_ref, sems = refs[n_copies + 6 :]
        y, z = place_ref[0], place_ref[1]
        copies = [(r, x_ref.at[place_ref[2 + i]]) for i, r in enumerate(token_refs)]
        at = 0
        for r, n in zip(weight_refs, cols):
            copies.append((r, w_ref.at[pl.ds(pl.multiple_of(z * kb, kb), kb), pl.ds(at, n)]))
            at += n
        for r, (s, j) in zip(piece_refs, order):
            start = ((z + n_z - s) % n_z) * kb + ((y + n_y - j) % n_y) * part
            copies.append((r, w_ref.at[pl.ds(pl.multiple_of(start, part), part), :]))
        fetch(copies, sems)

        def project(n, carry):
            cut = pl.ds(pl.multiple_of(n * TILE, TILE), TILE)
            acc = jnp.zeros((rows, TILE), jnp.float32)
            for i in range(n_t):
                acc = acc + dot(x_ref[i], w_ref[i * width : (i + 1) * width, cut])
            qkv_ref[:, cut] = acc.astype(jnp.bfloat16)
            return carry

        lax.fori_loop(0, total // TILE, project, 0)
        low = jnp.zeros((rows, lower_ref.shape[1]), jnp.float32)
        for i in range(n_t):
            low = low + dot(x_ref[i], lower_ref[i * width : (i + 1) * width, :])
        low_ref[...] = low.astype(jnp.bfloat16)

        def block(c, states):
            return scan_block(
                heads, c, states, qkv_ref, low_ref, up_ref, bias_ref, extra_ref, gain_ref, out_ref
            )

        start = tuple(jnp.zeros((DV, DK), jnp.float32) for _ in range(heads))
        lax.fori_loop(0, rows // CHUNK, block, start)

    return pl.pallas_call(
        body,
        in_specs=[SMEM] + [ANY] * n_copies + [VMEM] * 5,
        out_specs=VMEM,
        out_shape=jax.ShapeDtypeStruct((rows, heads * DV), jnp.bfloat16),
        scratch_shapes=[
            pltpu.VMEM((n_t, rows, width), jnp.bfloat16),
            pltpu.VMEM((kb * n_z, total), jnp.bfloat16),
            pltpu.VMEM((rows, total), jnp.bfloat16),
            pltpu.VMEM((rows, lower.shape[1]), jnp.bfloat16),
            pltpu.SemaphoreType.DMA((n_copies,)),
        ],
        cost_estimate=pl.CostEstimate(flops=2 * 10**9, bytes_accessed=8 * MIB, transcendentals=0),
        compiler_params=pltpu.CompilerParams(vmem_limit_bytes=32 * MIB),
    )(place, *tokens, *weights, *pieces, lower, up, bias, extra, gain)


def column_call(place, n_y, n_z, direct, left, own, own_rows, pieces, flops):
    m, k = left.shape
    cw = own.shape[1]
    part = k // n_y
    order = pieces_of(n_z, n_y)
    n_copies = 1 + len(order)
    n_half = n_z // CORES
    step = min(m, 512)

    def body(place_ref, left_ref, *refs):
        y, z, c = place_ref[0], place_ref[1], place_ref[2]
        piece_refs = refs[1:n_copies]
        outs = refs[n_copies:-2]
        w_ref, sems = refs[-2:]
        begin = pl.multiple_of(place_ref[3] * k, k)
        copies = [(refs[0].at[pl.ds(begin, k), :], w_ref.at[z])]
        for r, (s, j) in zip(piece_refs, order):
            start = pl.multiple_of(((y + n_y - j) % n_y) * part, part)
            copies.append((r, w_ref.at[(z + n_z - s) % n_z, pl.ds(start, part), :]))
        fetch(copies, sems)

        def one(index, carry):
            f, r = index // (m // step), index % (m // step)
            rows = pl.ds(pl.multiple_of(r * step, step), step)
            value = dot(left_ref[rows, :], w_ref[f]).astype(jnp.bfloat16)
            if direct:

                @pl.when(f % CORES == c)
                def _():
                    outs[0][f // CORES, rows, :] = value

                @pl.when(f % CORES != c)
                def _():
                    outs[1][f // CORES, rows, :] = value

            else:
                outs[0][f, rows, :] = value
            return carry

        lax.fori_loop(0, n_z * (m // step), one, 0)

    shapes = [(n_half, m, cw)] * 2 if direct else [(n_z, m, cw)]
    return pl.pallas_call(
        body,
        in_specs=[SMEM, VMEM] + [ANY] * n_copies,
        out_specs=[VMEM] * len(shapes),
        out_shape=[jax.ShapeDtypeStruct(s, jnp.bfloat16) for s in shapes],
        scratch_shapes=[
            pltpu.VMEM((n_z, k, cw), jnp.bfloat16),
            pltpu.SemaphoreType.DMA((n_copies,)),
        ],
        cost_estimate=pl.CostEstimate(flops=flops, bytes_accessed=8 * MIB, transcendentals=0),
        compiler_params=pltpu.CompilerParams(vmem_limit_bytes=32 * MIB),
    )(place, left, own, *pieces)


def up_call(place, n_y, n_z, n_t, blocks, gains, own, pieces):
    width = gains[0].shape[1]
    kb = own.shape[0]
    hidden = own.shape[1] // PAIR
    part = kb // n_y
    rows = sum(b.shape[0] for b, _, _ in blocks) // n_t
    order = pieces_of(n_z, n_y)
    n_b = len(blocks)
    n_copies = n_b + len(gains) + 1 + len(order)
    step = 256

    def body(place_ref, *refs):
        block_refs = refs[:n_b]
        gain_refs = refs[n_b : n_b + n_t]
        own_ref = refs[n_b + n_t]
        piece_refs = refs[n_b + n_t + 1 : n_copies]
        act_ref, local_ref = refs[n_copies : n_copies + 2]
        v_ref, g_ref, w_ref, sems = refs[n_copies + 2 :]
        y, z = place_ref[0], place_ref[1]
        copies = []
        for r, (array, slot, first) in zip(block_refs, blocks):
            copies.append((r, v_ref.at[place_ref[2 + slot], pl.ds(first, array.shape[0]), :]))
        for i, r in enumerate(gain_refs):
            copies.append((r, g_ref.at[place_ref[2 + i]]))
        cut = pl.ds(pl.multiple_of((z % PAIR) * hidden, hidden), hidden)
        copies.append((own_ref.at[:, cut], w_ref.at[pl.ds(pl.multiple_of(z * kb, kb), kb), :]))
        for r, (s, j) in zip(piece_refs, order):
            start = ((z + n_z - s) % n_z) * kb + ((y + n_y - j) % n_y) * part
            copies.append((r, w_ref.at[pl.ds(pl.multiple_of(start, part), part), :]))
        fetch(copies, sems)

        def one(r, carry):
            here = pl.ds(pl.multiple_of(r * step, step), step)
            total = jnp.zeros((step, 1), jnp.float32)
            square = jnp.zeros((step, 1), jnp.float32)
            for i in range(n_t):
                value = v_ref[i, here, :].astype(jnp.float32)
                total = total + jnp.sum(value, axis=1, keepdims=True)
                square = square + jnp.sum(value * value, axis=1, keepdims=True)
            mean = total / (n_t * width)
            scale = lax.rsqrt(square / (n_t * width) - mean * mean + EPS)
            for i in range(n_t):
                value = v_ref[i, here, :].astype(jnp.float32)
                v_ref[i, here, :] = ((value - mean) * scale * g_ref[i]).astype(jnp.bfloat16)
            for n in range(hidden // TILE):
                acc = jnp.zeros((step, TILE), jnp.float32)
                for i in range(n_t):
                    acc = acc + dot(
                        v_ref[i, here, :],
                        w_ref[i * width : (i + 1) * width, n * TILE : (n + 1) * TILE],
                    )
                act = jnp.square(jnp.maximum(acc, 0.0)).astype(jnp.bfloat16)
                act_ref[here, n * TILE : (n + 1) * TILE] = act
            return carry

        lax.fori_loop(0, rows // step, one, 0)
        local_ref[...] = v_ref[place_ref[2], : rows // PAIR, :]

    return pl.pallas_call(
        body,
        in_specs=[SMEM] + [ANY] * n_copies,
        out_specs=[VMEM] * 2,
        out_shape=[
            jax.ShapeDtypeStruct((rows, hidden), jnp.bfloat16),
            jax.ShapeDtypeStruct((rows // PAIR, width), jnp.bfloat16),
        ],
        scratch_shapes=[
            pltpu.VMEM((n_t, rows, width), jnp.bfloat16),
            pltpu.VMEM((n_t, 1, width), jnp.float32),
            pltpu.VMEM((kb * n_z, hidden), jnp.bfloat16),
            pltpu.SemaphoreType.DMA((n_copies,)),
        ],
        cost_estimate=pl.CostEstimate(flops=4 * 10**9, bytes_accessed=8 * MIB, transcendentals=0),
        compiler_params=pltpu.CompilerParams(vmem_limit_bytes=32 * MIB),
    )(place, *[b for b, _, _ in blocks], *gains, own, *pieces)


def solution(mesh):
    n_y, n_z, n_t = mesh.shape["grp"], mesh.shape["fs"], mesh.shape["tp"]
    n_x = n_t // CORES
    direct = n_z == n_t

    def x_blocks(block):
        return [block] + [shift(block, "tp", n_t, CORES * k) for k in range(1, n_x)]

    def y_pieces(piece):
        return [piece] + [shift(piece, "grp", n_y, j) for j in range(1, n_y)]

    def at(array, index):
        return lax.dynamic_index_in_dim(array, index, 0, False)

    def split_cores(terms, c):
        if direct:
            return terms
        rows = terms[0].shape[1]
        whole = terms[0].transpose(1, 0, 2).reshape(rows, n_x, CORES, -1)
        split = whole.transpose(2, 1, 0, 3)
        return at(split, c), at(split, 1 - c)

    def f32(array):
        return array.astype(jnp.float32)

    def bf16(array):
        return array.astype(jnp.bfloat16)

    def local(
        tokens,
        query_matrix,
        key_weight,
        value_weight,
        forget_lower_factor,
        decay_up,
        decay_bias,
        log_extra,
        head_gain,
        out_weight,
        mix_gain,
        up_weight,
        down_weight,
        out_gain,
    ):
        y, z, t = lax.axis_index("grp"), lax.axis_index("fs"), lax.axis_index("tp")
        x, c = t // CORES, t % CORES
        rows, width = tokens.shape
        half = rows // 2
        depth = width * n_t
        kb = query_matrix.shape[0]
        key_cols = query_matrix.shape[1]
        slots = [(t - CORES * k) % n_t ^ d for k in range(n_x) for d in range(CORES)]
        place = jnp.stack([y, z] + slots).astype(jnp.int32)

        part = kb // n_y
        moving = jnp.concatenate(
            [
                lax.dynamic_slice_in_dim(w, y * part, part, 0)
                for w in (query_matrix, key_weight, value_weight)
            ],
            axis=1,
        )
        part_o = out_weight.shape[0] // n_y
        moving_o = lax.dynamic_slice_in_dim(out_weight, y * part_o, part_o, 0)
        token_blocks, gain_blocks = [], []
        qkv_pieces, o_pieces = [], []
        for s in range(1, n_z):
            moving = shift(moving, "fs", n_z, 1)
            moving_o = shift(moving_o, "fs", n_z, 1)
            if s == 1:
                for block in x_blocks(tokens):
                    token_blocks += [block, swap(block, "tp", n_t)]
                for block in x_blocks(mix_gain[None]):
                    gain_blocks += [block, swap(block, "tp", n_t)]
            qkv_pieces += y_pieces(moving)
            o_pieces += y_pieces(moving_o)

        hidden = up_weight.shape[1] // PAIR
        pair_at = z % PAIR
        up_gate = after(up_weight, moving)
        up_sends = [
            lax.dynamic_slice(up_gate, (y * part, ((pair_at + p) % PAIR) * hidden), (part, hidden))
            for p in range(PAIR)
        ]
        up_got = [shift(up_sends[s % PAIR], "fs", n_z, s) for s in range(1, n_z)]
        up_pieces = [piece for got in up_got for piece in y_pieces(got)]

        local_up = lax.dynamic_slice_in_dim(decay_up, t * key_cols, key_cols, 1)
        local_bias = lax.dynamic_slice_in_dim(decay_bias, t * key_cols, key_cols, 0)
        mixed_heads = mixer_call(
            place,
            n_y,
            n_z,
            token_blocks,
            (query_matrix, key_weight, value_weight),
            qkv_pieces,
            forget_lower_factor,
            local_up,
            local_bias[None],
            log_extra,
            head_gain[None],
        )
        spot = jnp.stack([y, z, c, jnp.zeros_like(z)]).astype(jnp.int32)
        mix_terms = column_call(
            spot, n_y, n_z, direct, mixed_heads, out_weight, 0, o_pieces, 10**9
        )
        mine, given = split_cores(mix_terms, c)
        got = swap(given, "tp", n_t)
        summed = ALPHA * f32(tokens) + f32(at(mine, x)) + f32(at(got, x))
        for k in range(1, n_x):
            there = (x + k) % n_x
            sent = bf16(f32(at(mine, there)) + f32(at(got, there)))
            summed = summed + f32(shift(sent, "tp", n_t, CORES * k))

        own = bf16(summed)
        own_a, own_b = own[:half], own[half:]
        z_a = swap(own_a, "fs", n_z)
        x_b = x_blocks(own_b)
        x_a = x_blocks(jnp.concatenate((own_a, z_a)))
        z_b = swap(jnp.concatenate(x_b), "fs", n_z)
        blocks = []
        own_swapped = swap(own, "tp", n_t)
        blocks += [(own, 0, 0), (own_swapped, 1, 0)]
        blocks += [(z_a, 0, rows), (swap(z_a, "tp", n_t), 1, rows)]
        z_b_swapped = swap(z_b, "tp", n_t)
        for k in range(n_x):
            piece = slice(k * half, (k + 1) * half)
            blocks += [(z_b[piece], 2 * k, rows + half), (z_b_swapped[piece], 2 * k + 1, rows + half)]
        for k in range(1, n_x):
            for d, a, b in ((0, x_a[k], x_b[k]), (1, swap(x_a[k], "tp", n_t), swap(x_b[k], "tp", n_t))):
                blocks += [(a[:half], 2 * k + d, 0), (a[half:], 2 * k + d, rows), (b, 2 * k + d, half)]

        part_d = hidden // n_y
        down_gate = after(down_weight, z_b)
        down_sends = [
            lax.dynamic_slice_in_dim(
                down_gate, ((pair_at + p) % PAIR) * hidden + y * part_d, part_d, 0
            )
            for p in range(PAIR)
        ]
        down_got = [shift(down_sends[s % PAIR], "fs", n_z, s) for s in range(1, n_z)]
        down_pieces = [piece for got in down_got for piece in y_pieces(got)]

        act, normed_local = up_call(
            place, n_y, n_z, n_t, blocks, gain_blocks, up_weight, up_pieces
        )
        spot = jnp.stack([y, z, c, pair_at]).astype(jnp.int32)
        down_terms = column_call(
            spot, n_y, n_z, direct, act, down_weight, pair_at * hidden, down_pieces, 4 * 10**9
        )
        mine, given = split_cores(down_terms, c)
        got = swap(given, "tp", n_t)
        fold = (n_x, PAIR, 2, half, width)
        mine, got = mine.reshape(fold), got.reshape(fold)

        def both(index, r, h):
            return f32(at(mine[:, r, h], index)) + f32(at(got[:, r, h], index))

        z_got = swap(bf16(f32(mine[:, 1, 0]) + f32(got[:, 1, 0])), "fs", n_z)
        x_got = [
            shift(
                bf16(f32(at(mine[:, :, 1], (x + k) % n_x)) + f32(at(got[:, :, 1], (x + k) % n_x))),
                "tp",
                n_t,
                CORES * k,
            )
            for k in range(1, n_x)
        ]
        down_a = both(x, 0, 0) + f32(at(z_got, x))
        for k in range(1, n_x):
            there = (x + k) % n_x
            sent = bf16(both(there, 0, 0) + f32(at(z_got, there)))
            down_a = down_a + f32(shift(sent, "tp", n_t, CORES * k))
        down_b, other_b = both(x, 0, 1), both(x, 1, 1)
        for x_k in x_got:
            down_b, other_b = down_b + f32(x_k[0]), other_b + f32(x_k[1])
        down_b = down_b + f32(swap(bf16(other_b), "fs", n_z))
        final = ALPHA * f32(normed_local) + jnp.concatenate((down_a, down_b))
        stats = jnp.stack((jnp.sum(final, axis=1), jnp.sum(final * final, axis=1)))
        stats = stats + swap(stats, "tp", n_t)
        total = stats
        for k in range(1, n_x):
            total = total + shift(stats, "tp", n_t, CORES * k)
        mean = total[0] / depth
        var = total[1] / depth - mean * mean
        return bf16((final - mean[:, None]) * lax.rsqrt(var[:, None] + EPS) * out_gain)

    in_specs = (
        P(("grp", "fs"), "tp"),
        P("fs", "tp"),
        P("fs", "tp"),
        P("fs", "tp"),
        P(),
        P(),
        P(),
        P(("grp", "fs"), "tp"),
        P(),
        P("tp", "fs"),
        P("tp"),
        P("fs", "tp"),
        P("tp", "fs"),
        P("tp"),
    )
    out_specs = P(("grp", "fs"), "tp")
    return jax.shard_map(local, mesh=mesh, in_specs=in_specs, out_specs=out_specs, check_vma=False)
```
